32 devices in a mesh: ep: 8 (over z, x), tp: 4 (over y, core).
Axes of the slice: x: 2, y: 2, z: 4, core: 2. Of those that a mesh axis runs over, the one named last changes fastest.
Arguments:
- mixer_query: bfloat16 [2048, 2048], P('ep', 'tp'), may hold values from -6 to 6
- mixer_forget: bfloat16 [2048, 2048], P('ep', 'tp'), may hold values from -5.5 to 5.5
- mixer_value: bfloat16 [2048, 2048], P('ep', 'tp'), may hold values from -6 to 6
- mixer_gate: bfloat16 [2048, 2048], P('ep', 'tp'), may hold values from -6 to 6
- forget_floor: float32 [2048], P('tp'), may hold values from 0.88 to 1
- head_gain: float32 [128], replicated, may hold values from 0.1 to 1.9
- mixer_proj: bfloat16 [2048, 2048], P(None, 'tp'), may hold values from -0.125 to 0.125
- expert_tokens: bfloat16 [1024, 2048], P('ep'), may hold values from -6 to 6
- expert_gain: float32 [2048], replicated, may hold values from 0.1 to 1.9
- routes: int32 [1024, 2], P('ep'), may hold values from 0 to 7, as said below
- group_logits: float32 [1024, 4], P('ep'), may hold values from -6 to 6
- choice_logits: float32 [1024, 2], P('ep'), may hold values from -6 to 6
- w_gate: bfloat16 [8, 2048, 2048], P('ep', None, 'tp'), may hold values from -0.125 to 0.125
- w_up: bfloat16 [8, 2048, 2048], P('ep', None, 'tp'), may hold values from -0.125 to 0.125
- w_down: bfloat16 [8, 2048, 2048], P('ep', None, 'tp'), may hold values from -0.125 to 0.125
Outputs:
- mixer_out: bfloat16 [2048, 2048], P('ep', 'tp')
- expert_out: bfloat16 [1024, 2048], P('ep', 'tp')
The draws below stay inside these ranges and needn't reach their ends.
Inputs may be any that keep to these rules, and one draw needn't show every extreme that they name: `routes`: in each aligned block of 128 rows (the rows of one index of ep) no expert is named by more than 64 rows, and some expert reaches that bound in every block; the 2 experts of a row differ and lie in the same group.
All inputs are finite; a program needn't handle non-finite values.
Results may differ from the reference program's by a relative error of at most 0.01.
Values may be sent and summed in bfloat16 or wider, within the bound.
A program may use at most 64 MiB of HBM per device.

```python
import math
import jax
import jax.numpy as jnp
from jax import lax

D = 2048
HEADS = 16
KEYDIM = 128
VDIM = 128
FF = 2048
GROUPS = 4
TOPK = 2
BLOCK = 64
TOKA_DEV = 256
TOKB_DEV = 128
EXPERTS = 8
EXP_GROUP = 2
CAP = 64
TOKENS_A = 2048
TOKENS_B = 1024
N_EP = 8


def draw_mixer_forget(key, part):
    noise_key = jax.random.fold_in(key, 11)
    shift_key = jax.random.fold_in(key, 12)
    noise = jnp.clip(jax.random.normal(noise_key, (TOKENS_A, HEADS * KEYDIM), jnp.float32), -4.0, 4.0)
    shifts = jax.random.uniform(shift_key, (TOKENS_A // TOKA_DEV, 1, 1), jnp.float32, -1.5, 1.5)
    shaped = noise.reshape(TOKENS_A // TOKA_DEV, TOKA_DEV, HEADS * KEYDIM) + shifts
    return shaped.reshape(TOKENS_A, HEADS * KEYDIM).astype(jnp.bfloat16)


def draw_forget_floor(key, part):
    pick_key = jax.random.fold_in(key, 21)
    slow_key = jax.random.fold_in(key, 22)
    fast_key = jax.random.fold_in(key, 23)
    slow_share = 0.5
    slow_heads = jax.random.uniform(pick_key, (HEADS, 1), jnp.float32) < slow_share
    slow_gap = jax.random.uniform(slow_key, (HEADS, KEYDIM), jnp.float32, 0.3, 2.0) / TOKENS_A
    fast_gap = jnp.exp(jax.random.uniform(fast_key, (HEADS, KEYDIM), jnp.float32, math.log(0.03), math.log(0.12)))
    gap_rows = jnp.where(slow_heads, slow_gap, fast_gap)
    return (1.0 - gap_rows).reshape(HEADS * KEYDIM).astype(jnp.float32)


def route_block(block_key):
    group_size = EXPERTS // GROUPS
    quota = TOKB_DEV // EXPERTS
    expert_ids = jnp.arange(EXPERTS, dtype=jnp.int32)
    counts = jnp.full((EXPERTS,), quota, jnp.int32)
    counts = counts + quota * ((expert_ids == 0) | (expert_ids == group_size - 1)).astype(jnp.int32)
    counts = counts - quota * ((expert_ids == group_size) | (expert_ids == group_size + 1)).astype(jnp.int32)
    canonical = jnp.repeat(expert_ids, counts, total_repeat_length=TOKB_DEV)
    order = jax.random.permutation(jax.random.fold_in(block_key, 1), TOKB_DEV)
    first = canonical[order]
    second = first // group_size * group_size + (first % group_size + 1) % group_size
    group_map = jax.random.permutation(jax.random.fold_in(block_key, 2), GROUPS).astype(jnp.int32)
    rotation = jax.random.randint(jax.random.fold_in(block_key, 3), (GROUPS,), 0, group_size).astype(jnp.int32)

    def relabel(ids):
        grp = ids // group_size
        return (group_map[grp] * group_size + (ids % group_size + rotation[grp]) % group_size).astype(jnp.int32)
    first = relabel(first)
    second = relabel(second)
    flip = jax.random.randint(jax.random.fold_in(block_key, 4), (TOKB_DEV,), 0, 2).astype(jnp.int32)
    left = flip * second + (1 - flip) * first
    right = flip * first + (1 - flip) * second
    return jnp.stack([left, right], axis=-1).astype(jnp.int32)


def draw_routes(key, part):
    base_key = jax.random.fold_in(key, 31)
    block_keys = jax.vmap(lambda index: jax.random.fold_in(base_key, index))(jnp.arange(N_EP))
    return jax.vmap(route_block)(block_keys).reshape(TOKENS_B, TOPK).astype(jnp.int32)


def steps_of(key, extent, cuts, least, largest):
    gain, own = 1.0, jax.random.fold_in(key, 6)
    for position, blocks in cuts:
        steps = jnp.exp(jax.random.uniform(jax.random.fold_in(own, position), (blocks,), jnp.float32, least / len(cuts), largest / len(cuts)))
        gain = gain * jnp.repeat(steps, extent[position] // blocks).reshape([-1 if axis == position else 1 for axis in range(len(extent))])
    return gain


def bell_draw(rng, shape, scale, bound, cuts=(), kind=jnp.bfloat16):
    loudness = steps_of(rng, shape, cuts, -0.22, 0.18) if cuts else 1.0
    values = jax.random.normal(rng, shape, jnp.float32) * scale * loudness
    return jnp.minimum(jnp.maximum(values, -bound), bound).astype(kind)


def setup_inputs(seed: int = 0) -> dict:
    key_of = jax.random.split(jax.random.key(seed), 16)
    return {
        "mixer_query": bell_draw(key_of[0], (TOKENS_A, HEADS * KEYDIM), 1.0, 6.0, ((0, 8), (1, 4))),
        "mixer_forget": draw_mixer_forget(jax.random.fold_in(key_of[15], 71), 0),
        "mixer_value": bell_draw(key_of[2], (TOKENS_A, HEADS * VDIM), 1.0, 6.0, ((0, 8), (1, 4))),
        "mixer_gate": bell_draw(key_of[3], (TOKENS_A, HEADS * VDIM), 1.0, 6.0, ((0, 8), (1, 4))),
        "forget_floor": draw_forget_floor(jax.random.fold_in(key_of[15], 71), 0),
        "head_gain": jnp.clip(1.0 + 0.18 * jax.random.normal(key_of[5], (VDIM,), jnp.float32), 0.1, 1.9),
        "mixer_proj": bell_draw(key_of[6], (HEADS * VDIM, D), (HEADS * VDIM) ** -0.5, 0.125, ((1, 4),)),
        "expert_tokens": bell_draw(key_of[7], (TOKENS_B, D), 1.0, 6.0, ((0, 8),)),
        "expert_gain": jnp.clip(1.0 + 0.18 * jax.random.normal(key_of[8], (D,), jnp.float32), 0.1, 1.9),
        "routes": draw_routes(jax.random.fold_in(key_of[15], 71), 0),
        "group_logits": bell_draw(key_of[10], (TOKENS_B, GROUPS), 1.0, 6.0, ((0, 8),), jnp.float32),
        "choice_logits": bell_draw(key_of[11], (TOKENS_B, TOPK), 1.0, 6.0, ((0, 8),), jnp.float32),
        "w_gate": bell_draw(key_of[12], (EXPERTS, D, FF), D ** -0.5, 0.125, ((0, 8), (2, 4))),
        "w_up": bell_draw(key_of[13], (EXPERTS, D, FF), D ** -0.5, 0.125, ((0, 8), (2, 4))),
        "w_down": bell_draw(key_of[14], (EXPERTS, FF, D), FF ** -0.5, 0.125, ((0, 8), (2, 4))),
    }


norm_eps = 1e-06
highest_precision = lax.Precision.HIGHEST

def rms_scale(features, gain_vec):
    return features * lax.rsqrt(lax.optimization_barrier(jnp.mean(features * features, axis=-1, keepdims=True)) + norm_eps) * gain_vec

def block_terms(query_block, input_block, log_blk, value_block, carried_state):
    cumulative_log = jnp.cumsum(log_blk, axis=0)
    between_block_term = jnp.einsum('zug,ugr->zur', query_block * jnp.exp(cumulative_log), carried_state, precision=highest_precision)
    causal = jnp.tril(jnp.ones((query_block.shape[0], query_block.shape[0]), dtype=bool))[:, :, None, None]
    differ = cumulative_log[:, None] - cumulative_log[None, :]
    decays = jnp.exp(jnp.where(causal, differ, -jnp.inf))
    scores = lax.optimization_barrier(jnp.sum(query_block[:, None] * input_block[None, :] * decays, axis=-1))
    result = between_block_term + jnp.einsum('tsh,shv->thv', scores, value_block, precision=highest_precision)
    ending_log_decay = cumulative_log[-1]
    updated_state = jnp.exp(ending_log_decay)[..., None] * carried_state + jnp.einsum('twa,twr->war', input_block * jnp.exp(ending_log_decay[None] - cumulative_log), value_block, precision=highest_precision)
    return (updated_state, result, cumulative_log)

def mixer_part(mixer_query, mixer_forget, mixer_value, mixer_gate, forget_floor, head_gain, mixer_proj):
    length = mixer_query.shape[0]
    blocks = length // BLOCK

    def split_blocks(source_array, last_width):
        return source_array.reshape(blocks, BLOCK, HEADS, last_width)
    queries = jax.nn.silu(mixer_query.astype(jnp.float32))
    input_rates = (1.0 - forget_floor) * jax.nn.sigmoid(-mixer_forget.astype(jnp.float32))
    log_forget = jnp.log1p(-input_rates)
    value_rows = mixer_value.astype(jnp.float32)

    def advance(carried_state, block_inputs):
        query_block, input_block, value_block, log_blk = block_inputs
        updated_state, result, cumulative_log = block_terms(query_block, input_block, log_blk, value_block, carried_state)
        return (updated_state, result)
    initial = jnp.zeros((HEADS, KEYDIM, VDIM), jnp.float32)
    _, output_rows = lax.scan(advance, initial, (split_blocks(queries, KEYDIM), split_blocks(input_rates, KEYDIM), split_blocks(value_rows, VDIM), split_blocks(log_forget, KEYDIM)))
    output_rows = output_rows.reshape(length, HEADS, VDIM)
    gate_act = jax.nn.silu(mixer_gate.astype(jnp.float32)).reshape(length, HEADS, VDIM)
    gated_out = rms_scale(output_rows, head_gain) * gate_act
    mixed_heads = gated_out.reshape(length, HEADS * VDIM).astype(jnp.bfloat16)
    return jnp.dot(mixed_heads, mixer_proj, preferred_element_type=jnp.float32).astype(jnp.bfloat16)

def gate_weights(routes, group_logits, choice_logits, group_size):
    group_exp = jnp.exp(group_logits)
    group_prob = group_exp / lax.optimization_barrier(jnp.sum(group_exp, axis=-1, keepdims=True))
    groups_of = routes // group_size
    member = (groups_of[..., None] == jnp.arange(GROUPS, dtype=jnp.int32)).astype(jnp.float32)
    picked_prob = lax.optimization_barrier(jnp.sum(member * group_prob[:, None, :], axis=-1))
    choice_exp = jnp.exp(choice_logits)
    together = (groups_of[:, :, None] == groups_of[:, None, :]).astype(jnp.float32)
    within = lax.optimization_barrier(jnp.sum(together * choice_exp[:, None, :], axis=-1))
    return picked_prob * choice_exp / within

def rank_slots(flat_routes, per_block, expert_count):
    onehot = (flat_routes[:, None] == jnp.arange(expert_count, dtype=jnp.int32)).astype(jnp.int32)
    blocked = onehot.reshape(-1, per_block, expert_count)
    earlier = (jnp.cumsum(blocked, axis=1) - blocked).astype(jnp.int32)
    return lax.optimization_barrier(jnp.sum(earlier * blocked, axis=-1)).astype(jnp.int32).reshape(-1)

def expert_part(expert_tokens, expert_gain, routes, group_logits, choice_logits, w_gate, w_up, w_down):
    count_rows = expert_tokens.shape[0]
    normed = rms_scale(expert_tokens.astype(jnp.float32), expert_gain).astype(jnp.bfloat16)
    weights = gate_weights(routes, group_logits, choice_logits, EXP_GROUP)
    flat_routes = routes.reshape(-1)
    per_block = TOKB_DEV * TOPK
    ranks = rank_slots(flat_routes, per_block, EXPERTS)
    block_ids = (jnp.arange(flat_routes.shape[0], dtype=jnp.int32) // per_block).astype(jnp.int32)
    slot_of = (flat_routes * (N_EP * CAP) + block_ids * CAP + ranks).astype(jnp.int32)
    token_ids = (jnp.arange(flat_routes.shape[0], dtype=jnp.int32) // TOPK).astype(jnp.int32)
    token_of = jnp.full((EXPERTS * N_EP * CAP,), count_rows, jnp.int32).at[slot_of].set(token_ids)
    padded = jnp.concatenate([normed, jnp.zeros((1, D), jnp.bfloat16)], axis=0)

    def run_expert(operands):
        gate_mat, up_mat, down_mat, index_rows = operands
        chosen = padded[index_rows]
        gate_pre = jnp.dot(chosen, gate_mat, preferred_element_type=jnp.float32)
        up_pre = jnp.dot(chosen, up_mat, preferred_element_type=jnp.float32)
        hidden = (jax.nn.silu(gate_pre) * up_pre).astype(jnp.bfloat16)
        return jnp.dot(hidden, down_mat, preferred_element_type=jnp.float32).astype(jnp.bfloat16)
    output_rows = lax.map(run_expert, (w_gate, w_up, w_down, token_of.reshape(EXPERTS, N_EP * CAP)))
    picked = output_rows.reshape(-1, D)[slot_of].astype(jnp.float32) * weights.reshape(-1)[:, None]
    return lax.optimization_barrier(jnp.sum(picked.reshape(count_rows, TOPK, D), axis=1)).astype(jnp.bfloat16)

def reference(mixer_query, mixer_forget, mixer_value, mixer_gate, forget_floor, head_gain, mixer_proj, expert_tokens, expert_gain, routes, group_logits, choice_logits, w_gate, w_up, w_down):
    mixer_out = mixer_part(mixer_query, mixer_forget, mixer_value, mixer_gate, forget_floor, head_gain, mixer_proj)
    expert_out = expert_part(expert_tokens, expert_gain, routes, group_logits, choice_logits, w_gate, w_up, w_down)
    return (mixer_out, expert_out)
```

```python
import jax
import jax.numpy as jnp
from jax import lax
from jax.experimental import pallas as pl
from jax.experimental.pallas import tpu as pltpu
from jax.sharding import PartitionSpec as P

KEYDIM = 128
VDIM = 128
GROUPS = 4
TOPK = 2
PAD = 8
norm_eps = 1e-06
F32 = jnp.float32
BF16 = jnp.bfloat16
VM = pl.BlockSpec(memory_space=pltpu.VMEM)
SM = pl.BlockSpec(memory_space=pltpu.SMEM)


def tn_dot(a, b):
    return lax.dot_general(a, b, (((0,), (0,)), ((), ())), preferred_element_type=F32)


def nt_dot(a, b):
    return lax.dot_general(a, b, (((1,), (1,)), ((), ())), preferred_element_type=F32)


def silu(v):
    return v / (1.0 + jnp.exp(-v))


def local_kernel(q_ref, f_ref, v_ref, floor_ref, intra_ref, qexp_ref, pay_ref):
    length = q_ref.shape[0]
    rows = lax.broadcasted_iota(jnp.int32, (length, length), 0)
    cols = lax.broadcasted_iota(jnp.int32, (length, length), 1)
    causal = cols <= rows
    tril = causal.astype(F32)
    for h in range(q_ref.shape[1] // KEYDIM):
        at = slice(h * KEYDIM, (h + 1) * KEYDIM)
        floor = floor_ref[:, at]
        rates = (1.0 - floor) / (1.0 + jnp.exp(f_ref[:, at].astype(F32)))
        cum = jnp.dot(
            tril, jnp.log(1.0 - rates), precision=lax.Precision.HIGHEST,
            preferred_element_type=F32,
        )
        end = cum[length - 1 : length, :]
        qexp = (silu(q_ref[:, at].astype(F32)) * jnp.exp(cum)).astype(BF16)
        kexp = (rates * jnp.exp(-cum)).astype(BF16)
        kend = (rates * jnp.exp(end - cum)).astype(BF16)
        value = v_ref[:, at]
        scores = jnp.where(causal, nt_dot(qexp, kexp), 0.0).astype(BF16)
        intra_ref[:, at] = jnp.dot(scores, value, preferred_element_type=F32)
        qexp_ref[:, at] = qexp
        pay_ref[h, :VDIM, :] = tn_dot(value, kend).astype(BF16)
        pay_ref[h, VDIM:, :] = jnp.broadcast_to(jnp.exp(end), (PAD, KEYDIM)).astype(BF16)


def finish_kernel(me_ref, all_ref, intra_ref, qexp_ref, gate_ref, gain_ref, out_ref):
    me = me_ref[0]
    for h in range(intra_ref.shape[1] // VDIM):
        at = slice(h * VDIM, (h + 1) * VDIM)

        def one(p, state):
            decay = all_ref[p, h, VDIM:, :].astype(F32)[:1]
            return state * decay + all_ref[p, h, :VDIM, :].astype(F32)

        state = lax.fori_loop(0, me, one, jnp.zeros((VDIM, KEYDIM), F32))
        out = intra_ref[:, at] + nt_dot(qexp_ref[:, at], state.astype(BF16))
        scale = lax.rsqrt(jnp.mean(out * out, axis=-1, keepdims=True) + norm_eps)
        out_ref[:, at] = (
            out * scale * gain_ref[...] * silu(gate_ref[:, at].astype(F32))
        ).astype(BF16)


def dispatch_kernel(half_ref, x_ref, gain_ref, routes_ref, gl_ref, cl_ref, out_ref, wt_ref):
    rows, width = x_ref.shape
    slots = out_ref.shape[0]
    part = out_ref.shape[1]
    experts = half_ref.shape[0] - 1
    capacity = slots // experts
    group_size = experts // GROUPS
    route = [routes_ref[:, j : j + 1] for j in range(TOPK)]
    ids = lax.broadcasted_iota(jnp.int32, (rows, experts), 1)
    hot = [(r == ids).astype(F32) for r in route]
    t0 = lax.broadcasted_iota(jnp.int32, (rows, rows), 0)
    t1 = lax.broadcasted_iota(jnp.int32, (rows, rows), 1)
    before = jnp.dot(
        (t1 < t0).astype(BF16), sum(hot).astype(BF16), preferred_element_type=F32
    )
    group_exp = jnp.exp(gl_ref[...])
    group_prob = group_exp / jnp.sum(group_exp, axis=-1, keepdims=True)
    gids = lax.broadcasted_iota(jnp.int32, (rows, GROUPS), 1)
    member = [
        ((r >= gids * group_size) & (r < (gids + 1) * group_size)).astype(F32) for r in route
    ]
    choice = [jnp.exp(cl_ref[:, j : j + 1]) for j in range(TOPK)]
    slot_ids = lax.broadcasted_iota(jnp.int32, (rows, slots), 1)
    place = jnp.zeros((rows, slots), F32)
    weight = jnp.zeros((rows, slots), F32)
    for j in range(TOPK):
        rank = jnp.sum(before * hot[j], axis=-1, keepdims=True).astype(jnp.int32)
        mark = (slot_ids == route[j] * capacity + rank).astype(F32)
        within = sum(
            jnp.sum(member[j] * member[i], axis=-1, keepdims=True) * choice[i]
            for i in range(TOPK)
        )
        prob = jnp.sum(member[j] * group_prob, axis=-1, keepdims=True)
        place = place + mark
        weight = weight + mark * (prob * choice[j] / within)
    high = weight.astype(BF16)
    wt_ref[0] = high
    wt_ref[1] = (weight - high.astype(F32)).astype(BF16)
    x = x_ref[...].astype(F32)
    scale = lax.rsqrt(jnp.mean(x * x, axis=-1, keepdims=True) + norm_eps)
    cols = pl.ds(pl.multiple_of(half_ref[0] * part, part), part)
    normed = (x_ref[:, cols].astype(F32) * scale * gain_ref[:, cols]).astype(BF16)
    out_ref[...] = tn_dot(place.astype(BF16), normed).astype(BF16)


def return_kernel(wt_ref, back_ref, out_ref):
    back = back_ref[...]
    out_ref[...] = (
        jnp.dot(wt_ref[0], back, preferred_element_type=F32)
        + jnp.dot(wt_ref[1], back, preferred_element_type=F32)
    ).astype(BF16)


def cost(flops, size):
    return pl.CostEstimate(flops=flops, bytes_accessed=size, transcendentals=0)


def shaped(shape, kind):
    return jax.ShapeDtypeStruct(shape, kind)


def per_device(
    mixer_query, mixer_forget, mixer_value, mixer_gate, forget_floor, head_gain, mixer_proj,
    expert_tokens, expert_gain, routes, group_logits, choice_logits, w_gate, w_up, w_down,
):
    length, width = mixer_query.shape
    heads = width // KEYDIM
    experts = lax.axis_size("ep")
    tp = lax.axis_size("tp")
    rows, model = expert_tokens.shape
    capacity = 2 * TOPK * rows // experts
    slots = experts * capacity
    split = 2
    part = model // split
    which = lax.axis_index("tp") % split
    half = jnp.full((experts + 1,), 0, jnp.int32) + which

    outgoing, wt = pl.pallas_call(
        dispatch_kernel,
        name="dispatch",
        out_shape=(shaped((slots, part), BF16), shaped((2, rows, slots), BF16)),
        in_specs=[SM, VM, VM, VM, VM, VM],
        out_specs=(VM, VM),
        cost_estimate=cost(2 * rows * slots * part, 4000000),
    )(half, expert_tokens, expert_gain[None, :], routes, group_logits, choice_logits)
    arrived = lax.all_to_all(
        outgoing.reshape(experts, capacity, part), "ep", split_axis=0, concat_axis=0, tiled=True
    )

    intra, qexp, pay = pl.pallas_call(
        local_kernel,
        name="local_scan",
        out_shape=(
            shaped((length, width), F32),
            shaped((length, width), BF16),
            shaped((heads, VDIM + PAD, KEYDIM), BF16),
        ),
        in_specs=[VM] * 4,
        out_specs=(VM, VM, VM),
        cost_estimate=cost(3000000000, 4000000),
    )(mixer_query, mixer_forget, mixer_value, forget_floor[None, :])
    everyone = lax.all_gather(pay, "ep")
    place = lax.axis_index("ep").astype(jnp.int32).reshape(1)
    mixed = pl.pallas_call(
        finish_kernel,
        name="mixer_finish",
        out_shape=shaped((length, width), BF16),
        in_specs=[SM] + [VM] * 5,
        out_specs=VM,
        cost_estimate=cost(1000000000, 4000000),
    )(place, everyone, intra, qexp, mixer_gate, head_gain[None, :])
    mixed_all = lax.all_gather(mixed, "tp", axis=1, tiled=True)

    groups = [list(range(s, s + split)) for s in range(0, tp, split)]
    flat_in = lax.all_gather(
        arrived.reshape(slots, part), "tp", axis=1, tiled=True, axis_index_groups=groups
    )
    gate_pre = jnp.dot(flat_in, w_gate[0], preferred_element_type=F32)
    up_pre = jnp.dot(flat_in, w_up[0], preferred_element_type=F32)
    hidden = (jax.nn.silu(gate_pre) * up_pre).astype(BF16)
    hidden_all = lax.all_gather(hidden, "tp", axis=1, tiled=True)
    mixer_out = jnp.dot(mixed_all, mixer_proj, preferred_element_type=F32).astype(BF16)
    down = jnp.dot(hidden_all, w_down[0], preferred_element_type=F32).astype(BF16)
    back = lax.all_to_all(
        down.reshape(experts, capacity, -1), "ep", split_axis=0, concat_axis=0, tiled=True
    ).reshape(slots, -1)
    expert_out = pl.pallas_call(
        return_kernel,
        name="weigh",
        out_shape=shaped((rows, back.shape[1]), BF16),
        in_specs=[VM, VM],
        out_specs=VM,
        cost_estimate=cost(4 * rows * slots * back.shape[1], 1000000),
    )(wt, back)
    return (mixer_out, expert_out)


def solution(mesh):
    return jax.shard_map(
        per_device,
        mesh=mesh,
        in_specs=(
            P("ep", "tp"),
            P("ep", "tp"),
            P("ep", "tp"),
            P("ep", "tp"),
            P("tp"),
            P(),
            P(None, "tp"),
            P("ep", None),
            P(),
            P("ep", None),
            P("ep", None),
            P("ep", None),
            P("ep", None, "tp"),
            P("ep", None, "tp"),
            P("ep", None, "tp"),
        ),
        out_specs=(P("ep", "tp"), P("ep", "tp")),
        check_vma=False,
    )
```

```python
import jax
import jax.numpy as jnp
from jax import lax
from jax.experimental import pallas as pl
from jax.experimental.pallas import tpu as pltpu
from jax.sharding import PartitionSpec as P

KEYDIM = 128
VDIM = 128
GROUPS = 4
TOPK = 2
PAD = 8
norm_eps = 1e-06
F32 = jnp.float32
BF16 = jnp.bfloat16
VM = pl.BlockSpec(memory_space=pltpu.VMEM)
SM = pl.BlockSpec(memory_space=pltpu.SMEM)


def tn_dot(a, b):
    return lax.dot_general(a, b, (((0,), (0,)), ((), ())), preferred_element_type=F32)


def nt_dot(a, b):
    return lax.dot_general(a, b, (((1,), (1,)), ((), ())), preferred_element_type=F32)


def silu(v):
    return v / (1.0 + jnp.exp(-v))


def local_kernel(q_ref, f_ref, v_ref, floor_ref, intra_ref, qexp_ref, pay_ref):
    length = q_ref.shape[0]
    rows = lax.broadcasted_iota(jnp.int32, (length, length), 0)
    cols = lax.broadcasted_iota(jnp.int32, (length, length), 1)
    causal = cols <= rows
    tril = causal.astype(F32)
    for h in range(q_ref.shape[1] // KEYDIM):
        at = slice(h * KEYDIM, (h + 1) * KEYDIM)
        floor = floor_ref[:, at]
        rates = (1.0 - floor) / (1.0 + jnp.exp(f_ref[:, at].astype(F32)))
        cum = jnp.dot(
            tril, jnp.log(1.0 - rates), precision=lax.Precision.HIGHEST,
            preferred_element_type=F32,
        )
        end = cum[length - 1 : length, :]
        qexp = (silu(q_ref[:, at].astype(F32)) * jnp.exp(cum)).astype(BF16)
        kexp = (rates * jnp.exp(-cum)).astype(BF16)
        kend = (rates * jnp.exp(end - cum)).astype(BF16)
        value = v_ref[:, at]
        scores = jnp.where(causal, nt_dot(qexp, kexp), 0.0).astype(BF16)
        intra_ref[:, at] = jnp.dot(scores, value, preferred_element_type=F32)
        qexp_ref[:, at] = qexp
        pay_ref[h, :VDIM, :] = tn_dot(value, kend).astype(BF16)
        pay_ref[h, VDIM:, :] = jnp.broadcast_to(jnp.exp(end), (PAD, KEYDIM)).astype(BF16)


def finish_kernel(state_ref, intra_ref, qexp_ref, gate_ref, gain_ref, out_ref):
    for h in range(intra_ref.shape[1] // VDIM):
        at = slice(h * VDIM, (h + 1) * VDIM)

        out = intra_ref[:, at] + nt_dot(qexp_ref[:, at], state_ref[h, :VDIM, :])
        scale = lax.rsqrt(jnp.mean(out * out, axis=-1, keepdims=True) + norm_eps)
        out_ref[:, at] = (
            out * scale * gain_ref[...] * silu(gate_ref[:, at].astype(F32))
        ).astype(BF16)


def dispatch_kernel(half_ref, x_ref, gain_ref, routes_ref, gl_ref, cl_ref, out_ref, wt_ref):
    rows, width = x_ref.shape
    slots = out_ref.shape[0]
    part = out_ref.shape[1]
    experts = half_ref.shape[0] - 1
    capacity = slots // experts
    group_size = experts // GROUPS
    route = [routes_ref[:, j : j + 1] for j in range(TOPK)]
    ids = lax.broadcasted_iota(jnp.int32, (rows, experts), 1)
    hot = [(r == ids).astype(F32) for r in route]
    t0 = lax.broadcasted_iota(jnp.int32, (rows, rows), 0)
    t1 = lax.broadcasted_iota(jnp.int32, (rows, rows), 1)
    before = jnp.dot(
        (t1 < t0).astype(BF16), sum(hot).astype(BF16), preferred_element_type=F32
    )
    group_exp = jnp.exp(gl_ref[...])
    group_prob = group_exp / jnp.sum(group_exp, axis=-1, keepdims=True)
    gids = lax.broadcasted_iota(jnp.int32, (rows, GROUPS), 1)
    member = [
        ((r >= gids * group_size) & (r < (gids + 1) * group_size)).astype(F32) for r in route
    ]
    choice = [jnp.exp(cl_ref[:, j : j + 1]) for j in range(TOPK)]
    slot_ids = lax.broadcasted_iota(jnp.int32, (rows, slots), 1)
    place = jnp.zeros((rows, slots), F32)
    weight = jnp.zeros((rows, slots), F32)
    for j in range(TOPK):
        rank = jnp.sum(before * hot[j], axis=-1, keepdims=True).astype(jnp.int32)
        mark = (slot_ids == route[j] * capacity + rank).astype(F32)
        within = sum(
            jnp.sum(member[j] * member[i], axis=-1, keepdims=True) * choice[i]
            for i in range(TOPK)
        )
        prob = jnp.sum(member[j] * group_prob, axis=-1, keepdims=True)
        place = place + mark
        weight = weight + mark * (prob * choice[j] / within)
    high = weight.astype(BF16)
    wt_ref[0] = high
    wt_ref[1] = (weight - high.astype(F32)).astype(BF16)
    x = x_ref[...].astype(F32)
    scale = lax.rsqrt(jnp.mean(x * x, axis=-1, keepdims=True) + norm_eps)
    cols = pl.ds(pl.multiple_of(half_ref[0] * part, part), part)
    normed = (x_ref[:, cols].astype(F32) * scale * gain_ref[:, cols]).astype(BF16)
    out_ref[...] = tn_dot(place.astype(BF16), normed).astype(BF16)


def return_kernel(wt_ref, back_ref, out_ref):
    back = back_ref[...]
    out_ref[...] = (
        jnp.dot(wt_ref[0], back, preferred_element_type=F32)
        + jnp.dot(wt_ref[1], back, preferred_element_type=F32)
    ).astype(BF16)


def later_after(later, earlier):
    later = later.astype(F32)
    rows = lax.broadcasted_iota(jnp.int32, later.shape, 1)
    decay = later[:, VDIM : VDIM + 1, :]
    return (decay * earlier.astype(F32) + jnp.where(rows < VDIM, later, 0.0)).astype(BF16)


def prefix(pay, count):
    span = pay
    before = None
    step = 1
    while step < count:
        came = lax.ppermute(span, "ep", [(i, i + step) for i in range(count - step)])
        before = came if before is None else later_after(before, came)
        step *= 2
        if step < count:
            span = later_after(span, came)
    return jnp.zeros_like(pay) if before is None else before


def cost(flops, size):
    return pl.CostEstimate(flops=flops, bytes_accessed=size, transcendentals=0)


def shaped(shape, kind):
    return jax.ShapeDtypeStruct(shape, kind)


def per_device(
    mixer_query, mixer_forget, mixer_value, mixer_gate, forget_floor, head_gain, mixer_proj,
    expert_tokens, expert_gain, routes, group_logits, choice_logits, w_gate, w_up, w_down,
):
    length, width = mixer_query.shape
    heads = width // KEYDIM
    experts = lax.axis_size("ep")
    tp = lax.axis_size("tp")
    rows, model = expert_tokens.shape
    capacity = 2 * TOPK * rows // experts
    slots = experts * capacity
    split = 2
    part = model // split
    which = lax.axis_index("tp") % split
    half = jnp.full((experts + 1,), 0, jnp.int32) + which

    outgoing, wt = pl.pallas_call(
        dispatch_kernel,
        name="dispatch",
        out_shape=(shaped((slots, part), BF16), shaped((2, rows, slots), BF16)),
        in_specs=[SM, VM, VM, VM, VM, VM],
        out_specs=(VM, VM),
        cost_estimate=cost(2 * rows * slots * part, 4000000),
    )(half, expert_tokens, expert_gain[None, :], routes, group_logits, choice_logits)
    arrived = lax.all_to_all(
        outgoing.reshape(experts, capacity, part), "ep", split_axis=0, concat_axis=0, tiled=True
    )

    intra, qexp, pay = pl.pallas_call(
        local_kernel,
        name="local_scan",
        out_shape=(
            shaped((length, width), F32),
            shaped((length, width), BF16),
            shaped((heads, VDIM + PAD, KEYDIM), BF16),
        ),
        in_specs=[VM] * 4,
        out_specs=(VM, VM, VM),
        cost_estimate=cost(3000000000, 4000000),
    )(mixer_query, mixer_forget, mixer_value, forget_floor[None, :])
    entering = prefix(pay, experts)
    mixed = pl.pallas_call(
        finish_kernel,
        name="mixer_finish",
        out_shape=shaped((length, width), BF16),
        in_specs=[VM] * 5,
        out_specs=VM,
        cost_estimate=cost(1000000000, 4000000),
    )(entering, intra, qexp, mixer_gate, head_gain[None, :])

    arrived, mixed = lax.optimization_barrier((arrived, mixed))
    mixed_all = lax.all_gather(mixed, "tp", axis=1, tiled=True)
    own = arrived.reshape(slots, part)
    other = lax.ppermute(own, "tp", [(i, i ^ 1) for i in range(tp)])
    flat_in = jnp.concatenate(
        [jnp.where(which == 0, own, other), jnp.where(which == 0, other, own)], axis=1
    )
    gate_pre = jnp.dot(flat_in, w_gate[0], preferred_element_type=F32)
    up_pre = jnp.dot(flat_in, w_up[0], preferred_element_type=F32)
    hidden = (jax.nn.silu(gate_pre) * up_pre).astype(BF16)
    hidden_all = lax.all_gather(hidden, "tp", axis=1, tiled=True)
    mixer_out = jnp.dot(mixed_all, mixer_proj, preferred_element_type=F32).astype(BF16)
    down = jnp.dot(hidden_all, w_down[0], preferred_element_type=F32).astype(BF16)
    back = lax.all_to_all(
        down.reshape(experts, capacity, -1), "ep", split_axis=0, concat_axis=0, tiled=True
    ).reshape(slots, -1)
    expert_out = pl.pallas_call(
        return_kernel,
        name="weigh",
        out_shape=shaped((rows, back.shape[1]), BF16),
        in_specs=[VM, VM],
        out_specs=VM,
        cost_estimate=cost(4 * rows * slots * back.shape[1], 1000000),
    )(wt, back)
    return (mixer_out, expert_out)


def solution(mesh):
    return jax.shard_map(
        per_device,
        mesh=mesh,
        in_specs=(
            P("ep", "tp"),
            P("ep", "tp"),
            P("ep", "tp"),
            P("ep", "tp"),
            P("tp"),
            P(),
            P(None, "tp"),
            P("ep", None),
            P(),
            P("ep", None),
            P("ep", None),
            P("ep", None),
            P("ep", None, "tp"),
            P("ep", None, "tp"),
            P("ep", None, "tp"),
        ),
        out_specs=(P("ep", "tp"), P("ep", "tp")),
        check_vma=False,
    )
```

```python
import jax
import jax.numpy as jnp
from jax import lax
from jax.experimental import pallas as pl
from jax.experimental.pallas import tpu as pltpu
from jax.sharding import PartitionSpec as P

KEYDIM = 128
VDIM = 128
GROUPS = 4
TOPK = 2
PAD = 8
norm_eps = 1e-06
F32 = jnp.float32
BF16 = jnp.bfloat16
VM = pl.BlockSpec(memory_space=pltpu.VMEM)
SM = pl.BlockSpec(memory_space=pltpu.SMEM)


def tn_dot(a, b):
    return lax.dot_general(a, b, (((0,), (0,)), ((), ())), preferred_element_type=F32)


def nt_dot(a, b):
    return lax.dot_general(a, b, (((1,), (1,)), ((), ())), preferred_element_type=F32)


def silu(v):
    return v / (1.0 + jnp.exp(-v))


def local_kernel(q_ref, f_ref, v_ref, floor_ref, intra_ref, qexp_ref, pay_ref):
    length = q_ref.shape[0]
    rows = lax.broadcasted_iota(jnp.int32, (length, length), 0)
    cols = lax.broadcasted_iota(jnp.int32, (length, length), 1)
    causal = cols <= rows
    tril = causal.astype(F32)
    for h in range(q_ref.shape[1] // KEYDIM):
        at = slice(h * KEYDIM, (h + 1) * KEYDIM)
        floor = floor_ref[:, at]
        rates = (1.0 - floor) / (1.0 + jnp.exp(f_ref[:, at].astype(F32)))
        cum = jnp.dot(
            tril, jnp.log(1.0 - rates), precision=lax.Precision.HIGHEST,
            preferred_element_type=F32,
        )
        end = cum[length - 1 : length, :]
        qexp = (silu(q_ref[:, at].astype(F32)) * jnp.exp(cum)).astype(BF16)
        kexp = (rates * jnp.exp(-cum)).astype(BF16)
        kend = (rates * jnp.exp(end - cum)).astype(BF16)
        value = v_ref[:, at]
        scores = jnp.where(causal, nt_dot(qexp, kexp), 0.0).astype(BF16)
        intra_ref[:, at] = jnp.dot(scores, value, preferred_element_type=F32)
        qexp_ref[:, at] = qexp
        pay_ref[h, :VDIM, :] = tn_dot(value, kend).astype(BF16)
        pay_ref[h, VDIM:, :] = jnp.broadcast_to(jnp.exp(end), (PAD, KEYDIM)).astype(BF16)


def finish_kernel(state_ref, intra_ref, qexp_ref, gate_ref, gain_ref, out_ref):
    for h in range(intra_ref.shape[1] // VDIM):
        at = slice(h * VDIM, (h + 1) * VDIM)

        out = intra_ref[:, at] + nt_dot(qexp_ref[:, at], state_ref[h, :VDIM, :])
        scale = lax.rsqrt(jnp.mean(out * out, axis=-1, keepdims=True) + norm_eps)
        out_ref[:, at] = (
            out * scale * gain_ref[...] * silu(gate_ref[:, at].astype(F32))
        ).astype(BF16)


def dispatch_kernel(half_ref, x_ref, gain_ref, routes_ref, gl_ref, cl_ref, out_ref, wt_ref):
    rows, width = x_ref.shape
    slots = out_ref.shape[0]
    part = out_ref.shape[1]
    experts = half_ref.shape[0] - 1
    capacity = slots // experts
    group_size = experts // GROUPS
    t0 = lax.broadcasted_iota(jnp.int32, (rows, rows), 0)
    t1 = lax.broadcasted_iota(jnp.int32, (rows, rows), 1)

    def column(row):
        return jnp.sum(jnp.where(t0 == t1, row.astype(F32), 0.0), axis=-1, keepdims=True)

    route = [column(routes_ref[j : j + 1, :]).astype(jnp.int32) for j in range(TOPK)]
    ids = lax.broadcasted_iota(jnp.int32, (rows, experts), 1)
    hot = [(r == ids).astype(F32) for r in route]
    before = jnp.dot(
        (t1 < t0).astype(BF16), sum(hot).astype(BF16), preferred_element_type=F32
    )
    group_exp = [jnp.exp(column(gl_ref[g : g + 1, :])) for g in range(GROUPS)]
    group_sum = sum(group_exp)
    gids = lax.broadcasted_iota(jnp.int32, (rows, GROUPS), 1)
    member = [
        ((r >= gids * group_size) & (r < (gids + 1) * group_size)).astype(F32) for r in route
    ]
    choice = [jnp.exp(column(cl_ref[j : j + 1, :])) for j in range(TOPK)]
    slot_ids = lax.broadcasted_iota(jnp.int32, (rows, slots), 1)
    place = jnp.zeros((rows, slots), F32)
    weight = jnp.zeros((rows, slots), F32)
    for j in range(TOPK):
        rank = jnp.sum(before * hot[j], axis=-1, keepdims=True).astype(jnp.int32)
        mark = (slot_ids == route[j] * capacity + rank).astype(F32)
        within = sum(
            jnp.sum(member[j] * member[i], axis=-1, keepdims=True) * choice[i]
            for i in range(TOPK)
        )
        prob = sum(member[j][:, g : g + 1] * group_exp[g] for g in range(GROUPS)) / group_sum
        place = place + mark
        weight = weight + mark * (prob * choice[j] / within)
    high = weight.astype(BF16)
    wt_ref[0] = high
    wt_ref[1] = (weight - high.astype(F32)).astype(BF16)
    x = x_ref[...].astype(F32)
    scale = lax.rsqrt(jnp.mean(x * x, axis=-1, keepdims=True) + norm_eps)
    cols = pl.ds(pl.multiple_of(half_ref[0] * part, part), part)
    normed = (x_ref[:, cols].astype(F32) * scale * gain_ref[:, cols]).astype(BF16)
    out_ref[...] = tn_dot(place.astype(BF16), normed).astype(BF16)


def return_kernel(wt_ref, back_ref, out_ref):
    back = back_ref[...]
    out_ref[...] = (
        jnp.dot(wt_ref[0], back, preferred_element_type=F32)
        + jnp.dot(wt_ref[1], back, preferred_element_type=F32)
    ).astype(BF16)


def later_after(later, earlier):
    later = later.astype(F32)
    rows = lax.broadcasted_iota(jnp.int32, later.shape, 1)
    decay = later[:, VDIM : VDIM + 1, :]
    return (decay * earlier.astype(F32) + jnp.where(rows < VDIM, later, 0.0)).astype(BF16)


def prefix(pay, count):
    span = pay
    before = None
    step = 1
    while step < count:
        came = lax.ppermute(span, "ep", [(i, i + step) for i in range(count - step)])
        before = came if before is None else later_after(before, came)
        step *= 2
        if step < count:
            span = later_after(span, came)
    return jnp.zeros_like(pay) if before is None else before


def cost(flops, size):
    return pl.CostEstimate(flops=flops, bytes_accessed=size, transcendentals=0)


def shaped(shape, kind):
    return jax.ShapeDtypeStruct(shape, kind)


def per_device(
    mixer_query, mixer_forget, mixer_value, mixer_gate, forget_floor, head_gain, mixer_proj,
    expert_tokens, expert_gain, routes, group_logits, choice_logits, w_gate, w_up, w_down,
):
    length, width = mixer_query.shape
    heads = width // KEYDIM
    experts = lax.axis_size("ep")
    tp = lax.axis_size("tp")
    rows, model = expert_tokens.shape
    capacity = 2 * TOPK * rows // experts
    slots = experts * capacity
    split = 2
    part = model // split
    which = lax.axis_index("tp") % split
    half = jnp.full((experts + 1,), 0, jnp.int32) + which

    outgoing, wt = pl.pallas_call(
        dispatch_kernel,
        name="dispatch",
        out_shape=(shaped((slots, part), BF16), shaped((2, rows, slots), BF16)),
        in_specs=[SM, VM, VM, VM, VM, VM],
        out_specs=(VM, VM),
        cost_estimate=cost(2 * rows * slots * part, 4000000),
    )(half, expert_tokens, expert_gain[None, :], routes.T, group_logits.T, choice_logits.T)
    arrived = lax.all_to_all(
        outgoing.reshape(experts, capacity, part), "ep", split_axis=0, concat_axis=0, tiled=True
    )

    intra, qexp, pay = pl.pallas_call(
        local_kernel,
        name="local_scan",
        out_shape=(
            shaped((length, width), F32),
            shaped((length, width), BF16),
            shaped((heads, VDIM + PAD, KEYDIM), BF16),
        ),
        in_specs=[VM] * 4,
        out_specs=(VM, VM, VM),
        cost_estimate=cost(3000000000, 4000000),
    )(mixer_query, mixer_forget, mixer_value, forget_floor[None, :])
    arrived, pay = lax.optimization_barrier((arrived, pay))
    entering = prefix(pay, experts)
    mixed = pl.pallas_call(
        finish_kernel,
        name="mixer_finish",
        out_shape=shaped((length, width), BF16),
        in_specs=[VM] * 5,
        out_specs=VM,
        cost_estimate=cost(1000000000, 4000000),
    )(entering, intra, qexp, mixer_gate, head_gain[None, :])
    mixed_all = lax.all_gather(mixed, "tp", axis=1, tiled=True)

    own = arrived.reshape(slots, part)
    other = lax.ppermute(own, "tp", [(i, i ^ 1) for i in range(tp)])
    flat_in = jnp.concatenate(
        [jnp.where(which == 0, own, other), jnp.where(which == 0, other, own)], axis=1
    )
    gate_pre = jnp.dot(flat_in, w_gate[0], preferred_element_type=F32)
    up_pre = jnp.dot(flat_in, w_up[0], preferred_element_type=F32)
    hidden = (jax.nn.silu(gate_pre) * up_pre).astype(BF16)
    hidden_all = lax.all_gather(hidden, "tp", axis=1, tiled=True)
    mixer_out = jnp.dot(mixed_all, mixer_proj, preferred_element_type=F32).astype(BF16)
    down = jnp.dot(hidden_all, w_down[0], preferred_element_type=F32).astype(BF16)
    back = lax.all_to_all(
        down.reshape(experts, capacity, -1), "ep", split_axis=0, concat_axis=0, tiled=True
    ).reshape(slots, -1)
    expert_out = pl.pallas_call(
        return_kernel,
        name="weigh",
        out_shape=shaped((rows, back.shape[1]), BF16),
        in_specs=[VM, VM],
        out_specs=VM,
        cost_estimate=cost(4 * rows * slots * back.shape[1], 1000000),
    )(wt, back)
    return (mixer_out, expert_out)


def solution(mesh):
    return jax.shard_map(
        per_device,
        mesh=mesh,
        in_specs=(
            P("ep", "tp"),
            P("ep", "tp"),
            P("ep", "tp"),
            P("ep", "tp"),
            P("tp"),
            P(),
            P(None, "tp"),
            P("ep", None),
            P(),
            P("ep", None),
            P("ep", None),
            P("ep", None),
            P("ep", None, "tp"),
            P("ep", None, "tp"),
            P("ep", None, "tp"),
        ),
        out_specs=(P("ep", "tp"), P("ep", "tp")),
        check_vma=False,
    )
```
